128 devices in a mesh: rep: 2 (over z_hi), fs: 32 (over z_lo, y, x), tp: 2 (over core).
Axes of the slice: x: 4, y: 4, z: 4 (z_hi: 2, z_lo: 2; z = z_hi * 2 + z_lo), core: 2. Of those that a mesh axis runs over, the one named last changes fastest.
Arguments:
- tokens: bfloat16 [64, 512, 2048], P(('rep', 'fs'), 'tp'), may hold values from -6 to 6
- norm_first: bfloat16 [2048], replicated, may hold values from 0.099609375 to 1.8984375
- norm_mixer: bfloat16 [2048], replicated, may hold values from 0.099609375 to 1.8984375
- norm_second: bfloat16 [2048], replicated, may hold values from 0.099609375 to 1.8984375
- ffn_gate: bfloat16 [2048, 2816], P('fs', 'tp'), may hold values from -0.125 to 0.125
- ffn_up: bfloat16 [2048, 2816], P('fs', 'tp'), may hold values from -0.125 to 0.125
- ffn_down: bfloat16 [2816, 2048], P('tp', 'fs'), may hold values from -0.109375 to 0.109375
- conv_value: bfloat16 [2048, 512], P('fs', 'tp'), may hold values from -0.125 to 0.125
- conv_gate: bfloat16 [2048, 512], P('fs', 'tp'), may hold values from -0.125 to 0.125
- depthwise: bfloat16 [31, 512], P(None, 'tp'), may hold values from -1.5 to 1.5
- conv_gain: bfloat16 [512], P('tp'), may hold values from 0.099609375 to 1.8984375
- conv_out: bfloat16 [512, 2048], P('tp', 'fs'), may hold values from -0.25 to 0.25
Outputs:
- mixed: bfloat16 [64, 512, 2048], P(('rep', 'fs'), 'tp')
The draws below stay inside these ranges and needn't reach their ends.
All inputs are finite; a program needn't handle non-finite values.
Results may differ from the reference program's by a relative error of at most 0.0095.
Values may be sent and summed in bfloat16 or wider, within the bound.
No kernel may reach another device: no remote copies, remote signals or barrier semaphores. Data moves between devices by JAX's collectives and lax.ppermute only.
A program may use at most 128 MiB of HBM per device.

```python
import jax
import jax.numpy as jnp
from jax import lax

D = 2048
FF = 2816
CONV = 512
KSIZE = 31
LEN = 512
SEQS = 64
N_TP = 2


def draw_depthwise(key, part):
    first, second, third = jax.random.split(jax.random.fold_in(key, 7), 3)
    base = jnp.clip(jax.random.normal(first, (KSIZE, CONV), jnp.float32), -3.0, 3.0) * KSIZE ** (-0.5)
    flipped = jax.random.randint(second, (), 0, 2)
    channel = jnp.arange(CONV)
    upper = (channel >= CONV // 2).astype(jnp.int32)
    factor = jnp.where(upper == flipped, 0.5, 1.6)
    jitter = jnp.exp(jax.random.uniform(third, (CONV,), jnp.float32, -0.35, 0.35))
    return (base * (factor * jitter)[None, :]).astype(jnp.bfloat16)


def block_levels(rng, extent, cuts, least, high):
    def one(axis_at, shards_of):
        heights = jax.random.uniform(jax.random.fold_in(jax.random.fold_in(rng, 6), axis_at), (shards_of,), jnp.float32, least / len(cuts), high / len(cuts))
        return jnp.repeat(jnp.exp(heights), extent[axis_at] // shards_of).reshape((-1,) + (1,) * (len(extent) - axis_at - 1))

    loudness = one(*cuts[0])
    for cut in cuts[1:]:
        loudness = loudness * one(*cut)
    return loudness


def gaussian(own_key, shape, scale, bound, cuts=(), dtype=jnp.bfloat16):
    result = jax.random.normal(own_key, shape, jnp.float32) * scale
    if len(cuts) > 0:
        result = block_levels(own_key, shape, cuts, -0.22, 0.18) * result
    return jnp.clip(result, min=-bound, max=bound).astype(dtype)


def setup_inputs(seed: int = 0) -> dict:
    arg_keys = jax.random.split(jax.random.key(seed), 13)
    tokens = gaussian(arg_keys[0], (SEQS, LEN, D), 1.0, 6.0, ((0, 64), (1, 2)))
    norm_first = jnp.clip(1.0 + 0.18 * jax.random.normal(arg_keys[1], (D,), jnp.float32), 0.099609375, 1.8984375).astype(jnp.bfloat16)
    norm_mixer = jnp.clip(1.0 + 0.18 * jax.random.normal(arg_keys[2], (D,), jnp.float32), 0.099609375, 1.8984375).astype(jnp.bfloat16)
    norm_second = jnp.clip(1.0 + 0.18 * jax.random.normal(arg_keys[3], (D,), jnp.float32), 0.099609375, 1.8984375).astype(jnp.bfloat16)
    ffn_gate = gaussian(arg_keys[4], (D, FF), D ** -0.5, 0.125, ((0, 32), (1, 2)))
    ffn_up = gaussian(arg_keys[5], (D, FF), D ** -0.5, 0.125, ((0, 32), (1, 2)))
    ffn_down = gaussian(arg_keys[6], (FF, D), FF ** -0.5, 0.109375, ((0, 2), (1, 32)))
    conv_value = gaussian(arg_keys[7], (D, CONV), D ** -0.5, 0.125, ((0, 32), (1, 2)))
    conv_gate = gaussian(arg_keys[8], (D, CONV), D ** -0.5, 0.125, ((0, 32), (1, 2)))
    depthwise = draw_depthwise(jax.random.fold_in(arg_keys[12], 71), 0)
    conv_gain = jnp.clip(1.0 + 0.18 * jax.random.normal(arg_keys[10], (CONV,), jnp.float32), 0.099609375, 1.8984375).astype(jnp.bfloat16)
    conv_out = gaussian(arg_keys[11], (CONV, D), CONV ** -0.5, 0.25, ((0, 2), (1, 32)))
    return {"tokens": tokens, "norm_first": norm_first, "norm_mixer": norm_mixer, "norm_second": norm_second, "ffn_gate": ffn_gate, "ffn_up": ffn_up, "ffn_down": ffn_down, "conv_value": conv_value, "conv_gate": conv_gate, "depthwise": depthwise, "conv_gain": conv_gain, "conv_out": conv_out}


ROW_EPS = 0.05
CHAN_EPS = 0.02

def rms_rows(stream, gain_vec):
    square_mean = lax.optimization_barrier(jnp.mean(stream * stream, axis=-1, keepdims=True))
    return (stream * lax.rsqrt(square_mean + ROW_EPS) * gain_vec.astype(jnp.float32)).astype(jnp.bfloat16)

def block_sum(left, right, blocks):
    width = left.shape[1] // blocks
    running = jnp.zeros((left.shape[0], right.shape[1]), jnp.float32)
    for block in range(blocks):
        partial_value = jnp.dot(left[:, block * width:(block + 1) * width], right[block * width:(block + 1) * width], preferred_element_type=jnp.float32)
        running = running + lax.optimization_barrier(partial_value.astype(jnp.bfloat16)).astype(jnp.float32)
    return running

def causal_taps(glu, kernel):
    length = glu.shape[0]
    padded = jnp.pad(glu, ((KSIZE - 1, 0), (0, 0)))
    output = jnp.zeros_like(glu)
    for tap_index in range(KSIZE):
        output = output + padded[tap_index:tap_index + length] * kernel[tap_index]
    return output

def reference(tokens, norm_first, norm_mixer, norm_second, ffn_gate, ffn_up, ffn_down, conv_value, conv_gate, depthwise, conv_gain, conv_out):

    def feed(normed):
        gate_rows = jnp.dot(normed, ffn_gate, preferred_element_type=jnp.float32)
        up_rows = jnp.dot(normed, ffn_up, preferred_element_type=jnp.float32)
        hidden = (jax.nn.silu(gate_rows) * up_rows).astype(jnp.bfloat16)
        return block_sum(hidden, ffn_down, N_TP)

    def one_sequence(sequence):
        stream = sequence.astype(jnp.float32)
        stream = stream + 0.5 * feed(rms_rows(stream, norm_first))
        normed = rms_rows(stream, norm_mixer)
        values = jnp.dot(normed, conv_value, preferred_element_type=jnp.float32)
        gates = jnp.dot(normed, conv_gate, preferred_element_type=jnp.float32)
        glu = values * jax.nn.sigmoid(gates)
        conv = causal_taps(glu, depthwise.astype(jnp.float32))
        average = lax.optimization_barrier(jnp.mean(conv, axis=-1, keepdims=True))
        centred = conv - average
        spread = lax.optimization_barrier(jnp.mean(centred * centred, axis=-1, keepdims=True))
        activated = jax.nn.silu(centred * lax.rsqrt(spread + CHAN_EPS) * conv_gain.astype(jnp.float32)).astype(jnp.bfloat16)
        stream = stream + block_sum(activated, conv_out, N_TP)
        stream = stream + 0.5 * feed(rms_rows(stream, norm_second))
        return stream.astype(jnp.bfloat16)
    return lax.map(one_sequence, tokens)
```

```python
import jax
import jax.numpy as jnp
from jax import lax
from jax.sharding import PartitionSpec as P

ROW_EPS = 0.05
CHAN_EPS = 0.02
SWAP = [(0, 1), (1, 0)]


def other(x):
    return lax.ppermute(x, "tp", SWAP)


def rms_rows(stream, gain_vec):
    square_mean = jnp.mean(stream * stream, axis=-1, keepdims=True)
    return (stream * lax.rsqrt(square_mean + ROW_EPS) * gain_vec.astype(jnp.float32)).astype(
        jnp.bfloat16
    )


def dot(a, b):
    return jnp.dot(a, b, preferred_element_type=jnp.float32)


def dot_t(a, b):
    return lax.dot_general(a, b, (((1,), (1,)), ((), ())), preferred_element_type=jnp.float32)


def feed(normed, gate, up, down_a, down_b):
    cut = down_a.shape[1]
    rows = jnp.concatenate([normed, other(normed)], axis=0)
    hidden = (jax.nn.silu(dot(rows, gate)) * dot(rows, up)).astype(jnp.bfloat16)
    half = normed.shape[0]

    def down(part):
        return dot_t(part[:, :cut], down_a) + dot_t(part[:, cut:], down_b)

    theirs = down(hidden[half:]).astype(jnp.bfloat16)
    received = other(theirs)
    return down(hidden[:half]) + received.astype(jnp.float32)


def causal_taps(padded, kernel, length):
    output = jnp.zeros((length, padded.shape[1]), jnp.float32)
    for tap_index in range(kernel.shape[0]):
        output = output + padded[tap_index : tap_index + length] * kernel[tap_index]
    return output


def shards(
    tokens,
    norm_first,
    norm_mixer,
    norm_second,
    ffn_gate,
    ffn_up,
    ffn_down,
    conv_value,
    conv_gate,
    depthwise,
    conv_gain,
    conv_out,
):
    width = tokens.shape[-1]
    tp = lax.axis_index("tp")
    rep = lax.axis_index("rep")
    n = ffn_gate.shape[1]
    c = conv_value.shape[1]
    down_t = ffn_down.T
    out_t = conv_out.T
    total = 20 * 128
    a_down = total - n - 2 * c
    b_down = total - n - c
    part0 = jnp.concatenate([ffn_gate, conv_value, conv_gate, down_t[:, :a_down]], axis=1)
    part1 = jnp.concatenate([ffn_up, out_t, down_t[:, n - b_down :]], axis=1)
    mine = jnp.where(rep == 0, part0, part1)
    full = lax.all_gather(mine, ("rep", "fs"), axis=0, tiled=True)
    first, second = full[:width], full[width:]
    gate, up = first[:, :n], second[:, :n]
    down_a = first[:, n + 2 * c :]
    down_b = second[:, n + c + (a_down + b_down - n) :]
    value_gate = first[:, n : n + 2 * c]
    out_half = second[:, n : n + c]
    value_gate_o = other(value_gate)
    out_half_o = other(out_half)
    taps = jnp.concatenate([depthwise, conv_gain[None, :]], axis=0).astype(jnp.float32)
    taps_o = other(taps)

    stream = tokens.reshape(-1, width).astype(jnp.float32)
    length = stream.shape[0]
    stream = stream + 0.5 * feed(rms_rows(stream, norm_first), gate, up, down_a, down_b)

    normed = rms_rows(stream, norm_mixer)
    both, both_o = dot(normed, value_gate), dot(normed, value_gate_o)
    glu = jnp.concatenate(
        [both[:, :c] * jax.nn.sigmoid(both[:, c:]), both_o[:, :c] * jax.nn.sigmoid(both_o[:, c:])],
        axis=1,
    )
    kernel = jnp.concatenate([taps, taps_o], axis=1)
    reach = depthwise.shape[0] - 1
    tail = glu[length - reach :]
    swapped = jnp.concatenate([tail[:, c:], tail[:, :c]], axis=1)
    before = jnp.where(tp == 1, other(swapped), 0.0)
    conv = causal_taps(jnp.concatenate([before, glu], axis=0), kernel[:-1], length)
    average = jnp.mean(conv, axis=1, keepdims=True)
    centred = conv - average
    spread = jnp.mean(centred * centred, axis=1, keepdims=True)
    activated = jax.nn.silu(centred * lax.rsqrt(spread + CHAN_EPS) * kernel[-1]).astype(jnp.bfloat16)
    stream = stream + dot_t(activated[:, :c], out_half) + dot_t(activated[:, c:], out_half_o)

    stream = stream + 0.5 * feed(rms_rows(stream, norm_second), gate, up, down_a, down_b)
    return stream.astype(jnp.bfloat16).reshape(tokens.shape)


def solution(mesh):
    in_specs = (
        P(("rep", "fs"), "tp", None),
        P(),
        P(),
        P(),
        P("fs", "tp"),
        P("fs", "tp"),
        P("tp", "fs"),
        P("fs", "tp"),
        P("fs", "tp"),
        P(None, "tp"),
        P("tp"),
        P("tp", "fs"),
    )
    out_specs = P(("rep", "fs"), "tp", None)
    return jax.shard_map(shards, mesh=mesh, in_specs=in_specs, out_specs=out_specs, check_vma=False)
```

```python
import jax
import jax.numpy as jnp
from jax import lax
from jax.experimental import pallas as pl
from jax.experimental.pallas import tpu as pltpu
from jax.sharding import Mesh
from jax.sharding import PartitionSpec as P

ROW_EPS = 0.05
CHAN_EPS = 0.02
SWAP = [(0, 1), (1, 0)]
ALL = ("zh", "zl", "y", "x", "tp")
WIDE = (("x", "y", "z"), ("y", "z", "x"))
NARROW = ("z", "x", "y")
FIRST_WIDE, FIRST_NARROW = 896, 512
ANY = pl.BlockSpec(memory_space=pl.ANY)
SMEM = pl.BlockSpec(memory_space=pltpu.SMEM)


def other(x):
    return lax.ppermute(x, "tp", SWAP)


def from_ring(x, dims, offsets):
    pairs = []
    for z in range(4):
        for y in range(4):
            for x_ in range(4):
                for tp in range(2):
                    source = {"z": z, "y": y, "x": x_}
                    source[dims[tp]] = (source[dims[tp]] + offsets[tp]) % 4
                    at = ((source["z"] * 4 + source["y"]) * 4 + source["x"]) * 2 + tp
                    pairs.append((at, ((z * 4 + y) * 4 + x_) * 2 + tp))
    return lax.ppermute(x, ALL, pairs)


def copied(coords, pieces, outs, plan):
    count = len(pieces)

    def body(coords_ref, *refs):
        sems = refs[-1]
        where = {d: coords_ref[i] for i, d in enumerate(("x", "y", "z", "tp"))}
        made = refs[count:-1]
        for place, length, copies in plan(where, refs[:count]):

            def step(i, carry=0, copies=copies):
                for source, out, index in copies(i):
                    pltpu.make_async_copy(source, made[out].at[index], sems.at[out]).start()
                return carry

            def run(length=length, step=step):
                lax.fori_loop(0, length, step, 0) if length > 1 else step(0)

            if place is None:
                run()
            else:
                pl.when(where["tp"] == place)(run)
        for out, ref in enumerate(made):
            pltpu.make_async_copy(ref, ref, sems.at[out]).wait()

    return pl.pallas_call(
        body,
        in_specs=[SMEM] + [ANY] * count,
        out_specs=[ANY] * len(outs),
        out_shape=[pltpu.VMEM(s, jnp.bfloat16) for s in outs],
        scratch_shapes=[pltpu.SemaphoreType.DMA((len(outs),))],
        compiler_params=pltpu.CompilerParams(vmem_limit_bytes=1 << 20),
    )(coords, *pieces)


def packed(coords, gate, up, down_t, value, gates, out_t):
    rows = gate.shape[0]

    def plan(where, ins):
        half = pl.ds(pl.multiple_of(where["z"] // 2 * (rows // 2), rows // 2), rows // 2)
        every = slice(None)
        copies, at = [], 0
        for ref, width in zip(ins, (FIRST_WIDE, FIRST_WIDE, 768, 256, 256, 256)):
            copies.append((ref.at[half, pl.ds(0, width)], 0, (every, pl.ds(at, width))))
            at += width
        at = 0
        for ref, start in zip(ins, (FIRST_WIDE, FIRST_WIDE, 768)):
            width = ref.shape[1] - start
            copies.append((ref.at[:, pl.ds(start, width)], 1, (every, pl.ds(at, width))))
            at += width
        return [(None, 1, lambda i: copies)]

    outs = [(rows // 2, 3328), (rows, 1664)]
    arrays = (gate, up, down_t, value, gates, out_t)
    arrays = [pltpu.with_memory_space_constraint(x, pltpu.HBM) for x in arrays]
    return copied(coords, arrays, outs, plan)


def wide_at(where, phase):
    return jnp.where(where["tp"] == 0, where[WIDE[0][phase]], where[WIDE[1][phase]])


def in_order(at, pieces, first_out, cuts):
    for k, piece in enumerate(pieces):
        for out, (start, stop) in enumerate(zip(cuts, cuts[1:])):
            source = piece.at[..., pl.ds(start, stop - start)]
            yield source, first_out + out, (at + k) % len(pieces)


def ring_of(x, dims):
    return [x] + [from_ring(x, dims, (k, k)) for k in (1, 2, 3)]


def ring_passed_on(x, dims, ways):
    near = from_ring(x, dims, ways)
    far = from_ring(near, dims, ways)
    last = from_ring(x, dims, tuple((-w) % 4 for w in ways))
    return [x, near, far, last]


def by_way(pieces, way):
    return list(pieces) if way == 1 else [pieces[0], pieces[3], pieces[2], pieces[1]]


def in_rows(coords, wides, narrows, wide_way, narrow_ways, cuts):
    every, parts = slice(None), len(cuts) - 1

    def plan(where, ins):
        def cut(piece, at):
            for part, start, stop in zip(range(parts), cuts, cuts[1:]):
                yield piece.at[..., pl.ds(start, stop - start)], part, at

        def by_z(_):
            for k, piece in enumerate(by_way(ins[:4], wide_way)):
                z = (where["z"] + k) % 4
                yield from cut(piece, (z % 2, every, every, z // 2))

        def by_x(z):
            for k, piece in enumerate(by_way(ins[:4], wide_way)):
                yield from cut(piece.at[z], (z % 2, every, (where["x"] + k) % 4, z // 2))

        def by_y(way):
            def of(zl):
                for k, piece in enumerate(by_way(ins[4:], way)):
                    yield piece.at[:, zl], parts, (zl, (where["y"] + k) % 4)

            return of

        return [
            (0, 1, by_z),
            (1, 4, by_x),
            (0, 2, by_y(narrow_ways[0])),
            (1, 2, by_y(narrow_ways[1])),
        ]

    outs = [(2, 4, 4, 2, 32, b - a) for a, b in zip(cuts, cuts[1:])]
    outs.append((2, 4, 4, 64, narrows[0].shape[-1]))
    return [x.reshape(-1, x.shape[-1]) for x in copied(coords, (*wides, *narrows), outs, plan)]


def gathered(coords, wide, narrow):
    def dims(phase):
        return (WIDE[0][phase], WIDE[1][phase])

    def same(phase):
        return (NARROW[phase],) * 2

    hold = lax.optimization_barrier
    pieces = hold((*ring_of(wide, dims(0)), narrow, from_ring(narrow, same(0), (1, 3))))
    wide, narrow = hold(
        tuple(
            copied(
                coords,
                pieces,
                [(4, *wide.shape), (2, *narrow.shape)],
                lambda where, ins: [
                    (None, 1, lambda i: in_order(wide_at(where, 0), ins[:4], 0, (0, wide.shape[-1]))),
                    (None, 1, lambda i: in_order(where["z"] % 2, ins[4:], 1, (0, narrow.shape[-1]))),
                ],
            )
        )
    )
    pieces = hold((*ring_of(wide, dims(1)), *ring_of(narrow, same(1))))
    cut_wide, cut_narrow = 2 * FIRST_WIDE, 2 * FIRST_NARROW
    shapes = [
        (4, *wide.shape[:-1], cut_wide),
        (4, *wide.shape[:-1], wide.shape[-1] - cut_wide),
        (4, *narrow.shape[:-1], cut_narrow),
        (4, *narrow.shape[:-1], narrow.shape[-1] - cut_narrow),
    ]
    w0, w1, n0, n1 = hold(
        tuple(
            copied(
                coords,
                pieces,
                shapes,
                lambda where, ins: [
                    (None, 1, lambda i: in_order(wide_at(where, 1), ins[:4], 0, (0, cut_wide, wide.shape[-1]))),
                    (None, 1, lambda i: in_order(where["x"], ins[4:], 2, (0, cut_narrow, narrow.shape[-1]))),
                ],
            )
        )
    )
    w0 = ring_passed_on(w0, dims(2), (1, 1))
    w1 = ring_passed_on(w1, dims(2), (3, 3))
    n0 = ring_passed_on(n0, same(2), (1, 3))
    n1 = ring_passed_on(n1, same(2), (3, 1))
    first = in_rows(coords, w0, n0, 1, (1, 3), (0, cut_wide))
    second = in_rows(coords, w1, n1, 3, (3, 1), (0, 768, 1280, 1536))
    return first, second


def rms_rows(stream, gain_vec):
    square_mean = jnp.mean(stream * stream, axis=-1, keepdims=True)
    return (stream * lax.rsqrt(square_mean + ROW_EPS) * gain_vec.astype(jnp.float32)).astype(
        jnp.bfloat16
    )


def dot(a, b):
    return jnp.dot(a, b, preferred_element_type=jnp.float32)


def dot_t(a, b):
    return lax.dot_general(a, b, (((1,), (1,)), ((), ())), preferred_element_type=jnp.float32)


def hidden_units(rows, gate_ups):
    parts = []
    for gate_up in gate_ups:
        both = dot(rows, gate_up)
        n = both.shape[1] // 2
        parts.append((jax.nn.silu(both[:, :n]) * both[:, n:]).astype(jnp.bfloat16))
    return jnp.concatenate(parts, axis=1)


def down(hidden, downs):
    total, at = None, 0
    for weights in downs:
        n = weights.shape[1]
        part = dot_t(hidden[:, at : at + n], weights)
        total, at = part if total is None else total + part, at + n
    return total


def feed(normed, gate_ups, downs, together):
    length = normed.shape[0]
    if together:
        hidden = hidden_units(jnp.concatenate([normed, other(normed)], axis=0), gate_ups)
        mine, others = hidden[:length], hidden[length:]
    else:
        mine, others = (hidden_units(x, gate_ups) for x in (normed, other(normed)))
    received = other(down(others, downs).astype(jnp.bfloat16))
    return down(mine, downs) + received.astype(jnp.float32)


def causal_taps(padded, kernel, length):
    output = jnp.zeros((length, padded.shape[1]), jnp.float32)
    for tap_index in range(kernel.shape[0]):
        output = output + padded[tap_index : tap_index + length] * kernel[tap_index]
    return output


def shards(
    tokens,
    norm_first,
    norm_mixer,
    norm_second,
    ffn_gate,
    ffn_up,
    ffn_down,
    conv_value,
    conv_gate,
    depthwise,
    conv_gain,
    conv_out,
):
    width = tokens.shape[-1]
    tp = lax.axis_index("tp")
    coords = jnp.stack([lax.axis_index(a) for a in ("x", "y", ("zh", "zl"), "tp")]).astype(jnp.int32)
    c = conv_value.shape[1]
    wide, narrow = packed(coords, ffn_gate, ffn_up, ffn_down.T, conv_value, conv_gate, conv_out.T)
    gate_ups, (down_wide, value_gate, out_half, down_narrow) = gathered(coords, wide, narrow)
    downs = (down_wide, down_narrow)
    value_gate_o = other(value_gate)
    out_half_o = other(out_half)
    taps = jnp.concatenate([depthwise, conv_gain[None, :]], axis=0).astype(jnp.float32)
    taps_o = other(taps)

    stream = tokens.reshape(-1, width).astype(jnp.float32)
    length = stream.shape[0]
    stream = stream + 0.5 * feed(rms_rows(stream, norm_first), gate_ups, downs, True)

    normed = rms_rows(stream, norm_mixer)
    both, both_o = dot(normed, value_gate), dot(normed, value_gate_o)
    glu = jnp.concatenate(
        [both[:, :c] * jax.nn.sigmoid(both[:, c:]), both_o[:, :c] * jax.nn.sigmoid(both_o[:, c:])],
        axis=1,
    )
    kernel = jnp.concatenate([taps, taps_o], axis=1)
    reach = depthwise.shape[0] - 1
    tail = glu[length - reach :]
    swapped = jnp.concatenate([tail[:, c:], tail[:, :c]], axis=1)
    before = jnp.where(tp == 1, other(swapped), 0.0)
    conv = causal_taps(jnp.concatenate([before, glu], axis=0), kernel[:-1], length)
    average = jnp.mean(conv, axis=1, keepdims=True)
    centred = conv - average
    spread = jnp.mean(centred * centred, axis=1, keepdims=True)
    activated = jax.nn.silu(centred * lax.rsqrt(spread + CHAN_EPS) * kernel[-1]).astype(jnp.bfloat16)
    stream = stream + dot_t(activated[:, :c], out_half) + dot_t(activated[:, c:], out_half_o)

    stream = stream + 0.5 * feed(rms_rows(stream, norm_second), gate_ups, downs, False)
    return stream.astype(jnp.bfloat16).reshape(tokens.shape)


def solution(mesh):
    mesh = Mesh(mesh.devices.reshape(2, 2, 4, 4, 2), ("zh", "zl", "y", "x", "tp"))
    seqs, rows = ("zh", "zl", "y", "x"), ("zl", "y", "x")
    in_specs = (
        P(seqs, "tp", None),
        P(),
        P(),
        P(),
        P(rows, "tp"),
        P(rows, "tp"),
        P("tp", rows),
        P(rows, "tp"),
        P(rows, "tp"),
        P(None, "tp"),
        P("tp"),
        P("tp", rows),
    )
    out_specs = P(seqs, "tp", None)
    return jax.shard_map(shards, mesh=mesh, in_specs=in_specs, out_specs=out_specs, check_vma=False)
```
